32 devices in a mesh: ep: 16 (over z, y, x), tp: 2 (over core).
Axes of the slice: x: 2, y: 2, z: 4, core: 2. Of those that a mesh axis runs over, the one named last changes fastest.
Arguments:
- tokens: bfloat16 [4096, 1024], P('ep'), may hold values from -6 to 6
- norm_gain: float32 [1024], replicated, may hold values from 0.1 to 1.9
- routing: int32 [4096, 2], P('ep'), may hold values from 0 to 31, all different within a row; in each aligned block of 256 rows (0 to 255, 256 to 511, ...) at most 16 rows name the same one
- route_weights: float32 [4096, 2], P('ep'), may hold values from 0.1 to 1
- lengths: int32 [1024], P('ep'), may hold values from 1 to 4, 2560 in all
- w_gate: bfloat16 [32, 1024, 3584], P('ep', None, 'tp'), may hold values from -0.1875 to 0.1875
- w_up: bfloat16 [32, 1024, 3584], P('ep', None, 'tp'), may hold values from -0.1875 to 0.1875
- w_down: bfloat16 [32, 3584, 1024], P('ep', 'tp'), may hold values from -0.09375 to 0.09375
Outputs:
- mixed: bfloat16 [4096, 1024], P('ep', 'tp')
The draws below stay inside these ranges and needn't reach their ends.
Inputs may be any that keep to these rules, and one draw needn't show every extreme that they name: `routing`: each row names 2 different experts; at most 16 rows of one device name the same expert, and that many is reached.
All inputs are finite; a program needn't handle non-finite values. No bound on the sum of `lengths` on one device may be relied on, other than what follows from the above.
Results may differ from the reference program's by a relative error of at most 0.009.
Values may be sent and summed in bfloat16 or wider, within the bound.
A program may use at most 64 MiB of HBM per device.

```python
import math
import jax
import jax.numpy as jnp
import numpy as np
from jax import lax

D = 1024
FFE = 3584
TOPK = 2
SPAN = 4
TOK_DEV = 256
EXPERTS = 32
CAP = 16
SEQS = 1024
TOKENS = 4096
N_TP = 2


def block_scale(rng, shape, shards, least, top_value):
    factor_of, own = 1.0, jax.random.fold_in(rng, 6)
    for dim, shards_of in shards:
        steps = jnp.exp(jax.random.uniform(jax.random.fold_in(own, dim), (shards_of,), jnp.float32, least / len(shards), top_value / len(shards)))
        factor_of = factor_of * jnp.repeat(steps, shape[dim] // shards_of).reshape([-1 if axis == dim else 1 for axis in range(len(shape))])
    return factor_of


def length_profile(count, total, reach, skew):
    loads = [(1 << 20) // math.isqrt(standing ** skew) + 1 for standing in range(2, count + 1)]
    spare, given = total - reach - (count - 1), [1] * (count - 1)
    while spare > 0:
        candidates = [i for i in range(count - 1) if given[i] < reach]
        whole, remaining = sum([loads[i] for i in candidates]), spare
        for i in candidates:
            more = min(reach - given[i], max(1, remaining * loads[i] // whole), spare)
            given[i] = given[i] + more
            spare = spare - more
    return np.array([reach] + given)


def uneven_parts(stream_key, count, total, most, slope):
    if count == 2:
        one = jax.random.randint(stream_key, (), max(1, total - most), min(most, total - 1) + 1)
        return jnp.stack([one, total - one])
    sizes = jnp.asarray(length_profile(count, total, most, slope), jnp.int32)
    twos = (count - 1) // 2
    giver, receiver = sizes[1:1 + 2 * twos:2], sizes[2:2 + 2 * twos:2]
    room = jnp.minimum(giver - 1, most - receiver)
    passed = jax.random.randint(jax.random.fold_in(stream_key, 1), (twos,), 0, 1 << 20) % (room + 1)
    sizes = sizes.at[1:1 + 2 * twos:2].set(giver - passed).at[2:2 + 2 * twos:2].set(receiver + passed)
    return sizes[jax.random.permutation(jax.random.fold_in(stream_key, 2), count)]


def assign_block(stream_key, own, number, rows, count, top, reach, lean):
    order = jax.random.permutation(stream_key, count)
    heavy_load, ordinary = shares(count, rows * top, reach, lean, True), shares(count, rows * top, reach, lean, False)
    places = jnp.arange(count)

    def named(sizes, rotation):
        used = int((sizes > 0).sum())
        fixed = max(1, used // 4)
        shifted = fixed + (places - fixed + rotation * (used - fixed)) % max(1, count - fixed)
        return jnp.zeros((count,), jnp.int32).at[order[jnp.where(places < fixed, places, shifted)]].set(jnp.asarray(sizes, jnp.int32))

    sizes = jnp.where(number % 4 == 0, named(heavy_load, number // 4), named(ordinary, number - number // 4 - 1))
    mixed = jax.random.permutation(jax.random.fold_in(own, 3), count)
    source_of, sink = mixed[0:count // 2 * 2:2], mixed[1:count // 2 * 2:2]
    margin = jnp.minimum(sizes[source_of] - 1, reach - sizes[sink]) // 2
    margin = jnp.where((source_of == order[0]) | (sink == order[0]) | (sizes[sink] == 0), 0, jnp.maximum(margin, 0))
    shifted = jax.random.randint(jax.random.fold_in(own, 4), (count // 2,), 0, 1 << 20) % (margin + 1)
    sizes = sizes.at[source_of].add(-shifted).at[sink].add(shifted)
    members = jnp.searchsorted(jnp.cumsum(sizes), jnp.arange(rows * top), side="right").astype(jnp.int32)
    table = members.reshape(top, rows).T
    table = table[jax.random.permutation(jax.random.fold_in(own, 1), rows)]
    rotation = jax.random.randint(jax.random.fold_in(own, 2), (rows, 1), 0, top)
    return jnp.take_along_axis(table, (jnp.arange(top)[None, :] + rotation) % top, axis=1)


def shares(count, total, reach, slope, full):
    weights = [(1 << 20) // math.isqrt(grade ** slope) + 1 for grade in range(1, count + 1)]
    largest = reach if full else min(reach, max(-(-total // count), total * weights[0] // sum(weights)))
    least = 1 if total - largest >= count - 1 else 0
    holding, spare = [largest] + [least] * (count - 1), total - largest - least * (count - 1)
    while spare > 0:
        movable = [i for i in range(1, count) if holding[i] < largest] or [i for i in range(1, count) if holding[i] < reach]
        whole, remaining = sum([weights[i] for i in movable]), spare
        for i in movable:
            addition = min(reach - holding[i], max(1, remaining * weights[i] // whole), spare)
            holding[i] = holding[i] + addition
            spare = spare - addition
    return np.array(holding)


def bell_draw(rng, shape, deviation, most, split=(), kind=jnp.bfloat16):
    array = deviation * jax.random.normal(rng, shape, jnp.float32)
    if split:
        array = array * block_scale(rng, shape, split, -0.22, 0.18)
    return jnp.clip(array, -most, most).astype(kind)


def setup_inputs(seed: int = 0) -> dict:
    key_list = jax.random.split(jax.random.key(seed), 9)
    tokens = bell_draw(key_list[0], (TOKENS, D), 1.0, 6.0, ((0, 16),))
    norm_gain = jnp.clip(1.0 + 0.18 * jax.random.normal(key_list[1], (D,), jnp.float32), 0.1, 1.9)
    routing_keys = jax.random.split(jax.random.fold_in(key_list[2], 1), TOKENS // TOK_DEV)
    routing_turns = jax.random.permutation(jax.random.fold_in(key_list[2], 3), TOKENS // TOK_DEV)
    routing = jax.vmap(lambda own, number: assign_block(jax.random.fold_in(key_list[2], 2), own, number, TOK_DEV, EXPERTS, TOPK, CAP, 2))(routing_keys, routing_turns).reshape((TOKENS, TOPK))
    route_weights = jnp.clip(0.1 + 0.9 * jax.random.uniform(key_list[3], (TOKENS, TOPK), jnp.float32) ** block_scale(key_list[3], (TOKENS, TOPK), ((0, 16),), -0.2, 0.2), 0.1, 1.0)
    lengths = uneven_parts(key_list[4], SEQS, SEQS * 5 // 2, SPAN, 2).astype(jnp.int32)
    w_gate = bell_draw(key_list[5], (EXPERTS, D, FFE), D ** -0.5, 0.1875, ((0, 16), (2, 2)))
    w_up = bell_draw(key_list[6], (EXPERTS, D, FFE), D ** -0.5, 0.1875, ((0, 16), (2, 2)))
    w_down = bell_draw(key_list[7], (EXPERTS, FFE, D), FFE ** -0.5, 0.09375, ((0, 16), (1, 2)))
    return {"tokens": tokens, "norm_gain": norm_gain, "routing": routing, "route_weights": route_weights, "lengths": lengths, "w_gate": w_gate, "w_up": w_up, "w_down": w_down}


eps = 1e-06
block_rows = 64

def expert_rows(row_block, gate_mat, up_mat, down_mat):
    gate_proj = jnp.dot(row_block, gate_mat, preferred_element_type=jnp.float32)
    up_proj = jnp.dot(row_block, up_mat, preferred_element_type=jnp.float32)
    hidden = (jax.nn.silu(gate_proj) * up_proj).astype(jnp.bfloat16)
    half_width = FFE // N_TP
    summed = jnp.zeros((row_block.shape[0], D), jnp.float32)
    for core_part in range(N_TP):
        partial_value = jnp.dot(hidden[:, core_part * half_width:(core_part + 1) * half_width], down_mat[core_part * half_width:(core_part + 1) * half_width], preferred_element_type=jnp.float32)
        rounded = lax.optimization_barrier(partial_value.astype(jnp.bfloat16))
        summed = summed + rounded.astype(jnp.float32)
    return summed.astype(jnp.bfloat16)

def reference(tokens, norm_gain, routing, route_weights, lengths, w_gate, w_up, w_down):
    floats = tokens.astype(jnp.float32)
    normed = (floats * lax.rsqrt(lax.optimization_barrier(jnp.mean(floats * floats, axis=-1, keepdims=True)) + eps) * norm_gain).astype(jnp.bfloat16)
    position = jnp.arange(TOKENS, dtype=jnp.int32)
    live_rows = position % SPAN < lengths[position // SPAN]
    flat_ids = jnp.where(live_rows[:, None], routing, EXPERTS).reshape(-1).astype(jnp.int32)
    sorted_picks = jnp.argsort(flat_ids, stable=True).astype(jnp.int32)
    owner_rows = (sorted_picks // TOPK).astype(jnp.int32)
    weight_of = route_weights.reshape(-1)[sorted_picks]
    counts = lax.optimization_barrier(jnp.sum((flat_ids[:, None] == jnp.arange(EXPERTS, dtype=jnp.int32)[None, :]).astype(jnp.int32), axis=0))
    starts = (jnp.cumsum(counts) - counts).astype(jnp.int32)
    total_picks = TOKENS * TOPK

    def expert_step(expert, totals):
        gate_mat = w_gate[expert]
        up_mat = w_up[expert]
        down_mat = w_down[expert]
        first = starts[expert]
        amount = counts[expert]

        def has_more(carry_state):
            return carry_state[0] * block_rows < amount

        def block_step(carry_state):
            block_no, inner = carry_state
            pick_index = first + block_no * block_rows + jnp.arange(block_rows, dtype=jnp.int32)
            in_range = pick_index < first + amount
            clipped = jnp.minimum(pick_index, total_picks - 1).astype(jnp.int32)
            rows_at = owner_rows[clipped]
            result = expert_rows(normed[rows_at], gate_mat, up_mat, down_mat)
            factor = jnp.where(in_range, weight_of[clipped], 0.0)
            inner = inner.at[rows_at].add(factor[:, None] * result.astype(jnp.float32))
            return (block_no + 1, inner)
        ended = lax.while_loop(has_more, block_step, (jnp.int32(0), totals))
        return ended[1]
    totals = lax.fori_loop(0, EXPERTS, expert_step, jnp.zeros((TOKENS, D), jnp.float32))
    return totals.astype(jnp.bfloat16)
```

```python
import functools

import jax
import jax.numpy as jnp
from jax import lax
from jax.experimental import pallas as pl
from jax.experimental.pallas import tpu as pltpu
from jax.sharding import PartitionSpec as P

MESH = pl.DeviceIdType.MESH
PARTS = 4
ORDER = (0, 3, 1, 2)
TILE = 16
eps = 1e-06
BF = jnp.bfloat16
F32 = jnp.float32


def dot(a, b):
    return jnp.dot(a, b, preferred_element_type=F32)


def kernel(
    n, local, bound, span,
    gain_hbm, routing_hbm, weights_hbm, lengths_hbm,
    tokens_hbm, gate_hbm, up_hbm, down_hbm,
    out_ref,
    gain_ref, routing_ref, weights_ref, lengths_ref, tok, gate_w, up_w, down_w, outgoing, incoming, hidden, partial, theirs, returning, returned, comb,
    small_sem, tok_sem, w_sem, ready, disp_send, disp_recv, fwd_send, fwd_recv, part_send, part_recv, ret_send, ret_recv,
):
    me = lax.axis_index("ep")
    core = lax.axis_index("tp")
    other = 1 - core
    per = n // PARTS
    rows = per * bound
    slots = local * rows
    tok_rows, width = tok.shape
    half = width // 2
    chosen = routing_ref.shape[0]
    experts = n * local
    mine = pl.ds(pl.multiple_of(core * half, half), half)
    quarter = me // per
    inner = jnp.logical_or(quarter == 1, quarter == 2)

    def target(k):
        return lax.bitwise_xor(me, k)

    def members(q):
        return [k for k in range(q * per, (q + 1) * per) if k]

    small = [
        pltpu.make_async_copy(src, dst, small_sem.at[i])
        for i, (src, dst) in enumerate((
            (lengths_hbm, lengths_ref),
            (routing_hbm, routing_ref),
            (gain_hbm, gain_ref),
            (weights_hbm, weights_ref),
        ))
    ]
    tok_copy = pltpu.make_async_copy(tokens_hbm, tok, tok_sem)
    tok_copy.start()
    for copy in small:
        copy.start()

    barrier = pltpu.get_barrier_semaphore()

    def greet(sem, q):
        for k in members(q):
            pl.semaphore_signal(sem, inc=1, device_id=(target(k), core), device_id_type=MESH)

    pl.semaphore_signal(barrier, inc=1, device_id=(me, other), device_id_type=MESH)
    greet(barrier, 3)

    @pl.when(inner)
    def _():
        greet(barrier, 2)
        greet(barrier, 1)

    greet(barrier, 0)

    loads = {}
    for x in range(local):
        for i, (src, dst) in enumerate(((gate_hbm, gate_w), (up_hbm, up_w), (down_hbm, down_w))):
            loads[x, i] = pltpu.make_async_copy(src.at[x], dst.at[x], w_sem.at[x, i])
            loads[x, i].start()

    for copy in small:
        copy.wait()

    count = lengths_ref.shape[1]
    spread = (
        lax.broadcasted_iota(jnp.int32, (count, tok_rows), 1) // span
        == lax.broadcasted_iota(jnp.int32, (count, tok_rows), 0)
    ).astype(BF)
    lens = jnp.broadcast_to(lengths_ref[...].astype(F32), (8, count)).astype(BF)
    live_len = dot(lens, spread)[0:1]
    place = lax.broadcasted_iota(jnp.int32, (1, tok_rows), 1) % span
    live = place.astype(F32) < live_len
    routing = routing_ref[...]
    ids = lax.broadcasted_iota(jnp.int32, (experts, tok_rows), 0)
    named = ids == routing[0:1]
    for i in range(1, chosen):
        named = named | (ids == routing[i : i + 1])
    named = named & live
    earlier = (
        lax.broadcasted_iota(jnp.int32, (tok_rows, tok_rows), 0)
        < lax.broadcasted_iota(jnp.int32, (tok_rows, tok_rows), 1)
    ).astype(BF)
    rank = dot(jnp.where(named, 1.0, 0.0).astype(BF), earlier)
    rank = jnp.where(named, rank, -1.0).astype(BF)

    def slot_ids(shape, q):
        s = lax.broadcasted_iota(jnp.int32, shape, 0)
        k = (s // bound) % per + q * per
        peer = lax.bitwise_xor(jnp.full(shape, me, jnp.int32), k)
        return peer * local + s // rows, s % bound

    def find(q):
        owner, slot = slot_ids((slots, experts), q)
        to_expert = (owner == lax.broadcasted_iota(jnp.int32, (slots, experts), 1)).astype(BF)
        owner, slot = slot_ids((slots, tok_rows), q)
        return owner, dot(to_expert, rank) == slot.astype(F32)

    tok_copy.wait()
    floats = tok[...].astype(F32)
    scale = lax.rsqrt(jnp.mean(floats * floats, axis=-1, keepdims=True) + eps)
    normed = (tok[:, mine].astype(F32) * scale * gain_ref[:, mine]).astype(BF)

    def remote(src, dst, send, recv, device):
        return pltpu.make_async_remote_copy(
            src_ref=src, dst_ref=dst, send_sem=send, recv_sem=recv,
            device_id=device, device_id_type=MESH,
        )

    partner = (me, other)

    def landed(ref, q):
        return ref.at[q, :, 1:] if q == 0 else ref.at[q]

    def dispatch(k):
        q, j = k // per, k % per
        return remote(
            outgoing.at[q, :, j], incoming.at[q, :, j, :, mine],
            disp_send.at[q], disp_recv.at[q], (target(k), core),
        )

    def forward(q):
        view = incoming.at[q, :, :, :, mine]
        return remote(view, view, fwd_send.at[q], fwd_recv.at[q], partner)

    def swap(q, x):
        return remote(
            partial.at[q, x, other], theirs.at[q, x],
            part_send.at[q, x], part_recv.at[q, x], partner,
        )

    def give_back(k, x):
        q, j = k // per, k % per
        return remote(
            returning.at[q, x, j], returned.at[q, x, j],
            ret_send.at[q], ret_recv.at[q], (target(k), core),
        )

    def fill(q):
        hit = find(q)[1]
        block = dot(jnp.where(hit, 1.0, 0.0).astype(BF), normed).astype(BF)
        block = block.reshape(local, per, bound, half)
        outgoing[q] = block
        if q == 0:
            incoming[0, :, 0, :, mine] = block[:, 0]

    def send(q):
        for k in reversed(members(q)):
            dispatch(k).start()

    fill(3)
    pl.semaphore_wait(barrier, jnp.where(inner, 2 * per, 4 * per))

    @pl.when(jnp.logical_not(inner))
    def _():
        greet(ready, 1)
        greet(ready, 2)

    send(3)
    fill(0)
    send(0)
    fill(1)
    fill(2)
    for q in range(PARTS):
        owner, hit = find(q)
        value = jnp.zeros((slots, tok_rows), F32)
        for i in range(chosen):
            value = jnp.where(owner == routing[i : i + 1], weights_ref[i : i + 1], value)
        comb[q] = jnp.where(hit, value, 0.0).T

    @pl.when(inner)
    def _():
        pl.semaphore_wait(ready, 2 * per)

    send(1)
    send(2)

    def arrive(q):
        view = landed(incoming, q).at[..., mine]
        remote(view, view, disp_send.at[q], disp_recv.at[q], partner).wait_recv()
        forward(q).start()

    def finish(q, x):
        swap(q, x).wait_recv()
        total = (partial[q, x, core].astype(F32) + theirs[q, x].astype(F32)).astype(BF)
        total = total.reshape(per, bound, half)
        returning[q, x] = total
        if q == 0:
            returned[0, x, 0] = total[0]
        for k in reversed(members(q)):
            give_back(k, x).start()

    arrive(ORDER[0])
    pending = None
    first = True
    for i, q in enumerate(ORDER):
        forward(q).wait_recv()
        for x in range(local):
            xs = incoming[q, x].reshape(rows, width)
            if first:
                loads[x, 0].wait()
            gate = dot(xs, gate_w[x])
            if first:
                loads[x, 1].wait()
            hidden[...] = (gate / (1.0 + jnp.exp(-gate)) * dot(xs, up_w[x])).astype(BF)
            if first:
                loads[x, 2].wait()
            if pending:
                finish(*pending)
            down = dot(hidden[...], down_w[x]).astype(BF)
            partial[q, x, 0] = down[:, :half]
            partial[q, x, 1] = down[:, half:]
            swap(q, x).start()
            pending = (q, x)
        first = False
        if i + 1 < PARTS:
            arrive(ORDER[i + 1])
    finish(*pending)

    mixed = jnp.zeros((tok_rows, half), F32)
    for q in (0, 1, 3, 2):
        view = landed(returned, q)
        remote(view, view, ret_send.at[q], ret_recv.at[q], partner).wait_recv()
        values = returned[q].reshape(slots, half)
        weight = comb[q]
        high = weight.astype(BF)
        low = (weight - high.astype(F32)).astype(BF)
        mixed = mixed + dot(high, values) + dot(low, values)
    out_ref[...] = mixed.astype(BF)
    for q in range(PARTS):
        view = landed(outgoing, q)
        remote(view, view, disp_send.at[q], disp_recv.at[q], partner).wait_send()
        view = landed(returning, q)
        remote(view, view, ret_send.at[q], ret_recv.at[q], partner).wait_send()
        forward(q).wait_send()
        for x in range(local):
            swap(q, x).wait_send()


def per_device(n, tokens, norm_gain, routing, route_weights, lengths, w_gate, w_up, w_down):
    local, width, units = w_gate.shape
    tok_rows, chosen = routing.shape
    experts = n * local
    bound = 2 * ((tok_rows * chosen + 2 * experts - 1) // (2 * experts))
    bound = (bound + TILE - 1) // TILE * TILE
    half = width // 2
    per = n // PARTS
    rows = per * bound
    span = tok_rows // lengths.shape[0]
    vmem = pl.BlockSpec(memory_space=pltpu.VMEM)
    hbm = pl.BlockSpec(memory_space=pltpu.HBM)
    dma = pltpu.SemaphoreType.DMA
    return pl.pallas_call(
        functools.partial(kernel, n, local, bound, span),
        out_shape=pltpu.VMEM((tok_rows, half), BF),
        in_specs=[hbm] * 8,
        out_specs=vmem,
        scratch_shapes=[
            pltpu.VMEM((1, width), F32),
            pltpu.VMEM((chosen, tok_rows), jnp.int32),
            pltpu.VMEM((chosen, tok_rows), F32),
            pltpu.VMEM((1, lengths.shape[0]), jnp.int32),
            pltpu.VMEM((tok_rows, width), BF),
            pltpu.VMEM((local, width, units), BF),
            pltpu.VMEM((local, width, units), BF),
            pltpu.VMEM((local, units, width), BF),
            pltpu.VMEM((PARTS, local, per, bound, half), BF),
            pltpu.VMEM((PARTS, local, per, bound, width), BF),
            pltpu.VMEM((rows, units), BF),
            pltpu.VMEM((PARTS, local, 2, rows, half), BF),
            pltpu.VMEM((PARTS, local, rows, half), BF),
            pltpu.VMEM((PARTS, local, per, bound, half), BF),
            pltpu.VMEM((PARTS, local, per, bound, half), BF),
            pltpu.VMEM((PARTS, tok_rows, local * rows), F32),
            dma((4,)),
            dma,
            dma((local, 3)),
            pltpu.SemaphoreType.REGULAR,
            dma((PARTS,)),
            dma((PARTS,)),
            dma((PARTS,)),
            dma((PARTS,)),
            dma((PARTS, local)),
            dma((PARTS, local)),
            dma((PARTS,)),
            dma((PARTS,)),
        ],
        compiler_params=pltpu.CompilerParams(
            collective_id=0, has_side_effects=True, vmem_limit_bytes=66000000
        ),
    )(
        norm_gain.reshape(1, width),
        routing.T,
        route_weights.T,
        lengths.reshape(1, -1),
        tokens,
        w_gate,
        w_up,
        w_down,
    )


def solution(mesh):
    placed = (
        P("ep", None),
        P(),
        P("ep", None),
        P("ep", None),
        P("ep"),
        P("ep", None, "tp"),
        P("ep", None, "tp"),
        P("ep", "tp", None),
    )
    return jax.shard_map(
        functools.partial(per_device, mesh.shape["ep"]),
        mesh=mesh, in_specs=placed, out_specs=P("ep", "tp"), check_vma=False,
    )
```

```python
import functools

import jax
import jax.numpy as jnp
from jax import lax
from jax.experimental import pallas as pl
from jax.experimental.pallas import tpu as pltpu
from jax.sharding import PartitionSpec as P

MESH = pl.DeviceIdType.MESH
PARTS = 4
GROUPS = ((0, 3), (1, 2))
PLACE = {q: (g, i) for g, qs in enumerate(GROUPS) for i, q in enumerate(qs)}
TILE = 16
eps = 1e-06
BF = jnp.bfloat16
F32 = jnp.float32


def dot(a, b):
    return jnp.dot(a, b, preferred_element_type=F32)


def kernel(
    n, local, bound, span,
    gain_hbm, routing_hbm, weights_hbm, lengths_hbm,
    tokens_hbm, gate_hbm, up_hbm, down_hbm,
    out_ref,
    gain_ref, routing_ref, weights_ref, lengths_ref, tok, gate_w, up_w, down_w, outgoing, incoming, hidden, partial, theirs, returning, returned, comb,
    small_sem, tok_sem, w_sem, ready, disp_send, disp_recv, fwd_send, fwd_recv, part_send, part_recv, ret_send, ret_recv,
):
    me = lax.axis_index("ep")
    core = lax.axis_index("tp")
    other = 1 - core
    per = n // PARTS
    rows = per * bound
    slots = local * rows
    most = hidden.shape[0]
    tok_rows, width = tok.shape
    half = width // 2
    chosen = routing_ref.shape[0]
    experts = n * local
    mine = pl.ds(pl.multiple_of(core * half, half), half)
    quarter = me // per
    inner = jnp.logical_or(quarter == 1, quarter == 2)

    def target(k):
        return lax.bitwise_xor(me, k)

    def members(q):
        return [k for k in range(q * per, (q + 1) * per) if k]

    small = [
        pltpu.make_async_copy(src, dst, small_sem.at[i])
        for i, (src, dst) in enumerate((
            (lengths_hbm, lengths_ref),
            (routing_hbm, routing_ref),
            (gain_hbm, gain_ref),
            (weights_hbm, weights_ref),
        ))
    ]
    tok_copy = pltpu.make_async_copy(tokens_hbm, tok, tok_sem)
    tok_copy.start()
    for copy in small:
        copy.start()

    barrier = pltpu.get_barrier_semaphore()

    def greet(sem, q):
        for k in members(q):
            pl.semaphore_signal(sem, inc=1, device_id=(target(k), core), device_id_type=MESH)

    pl.semaphore_signal(barrier, inc=1, device_id=(me, other), device_id_type=MESH)
    greet(barrier, 3)

    @pl.when(inner)
    def _():
        greet(barrier, 2)
        greet(barrier, 1)

    greet(barrier, 0)

    loads = {}
    for x in range(local):
        for i, (src, dst) in enumerate(((gate_hbm, gate_w), (up_hbm, up_w), (down_hbm, down_w))):
            loads[x, i] = pltpu.make_async_copy(src.at[x], dst.at[x], w_sem.at[x, i])
            loads[x, i].start()

    for copy in small:
        copy.wait()
    tok_copy.wait()

    count = lengths_ref.shape[1]
    spread = (
        lax.broadcasted_iota(jnp.int32, (count, tok_rows), 1) // span
        == lax.broadcasted_iota(jnp.int32, (count, tok_rows), 0)
    ).astype(BF)
    lens = jnp.broadcast_to(lengths_ref[...].astype(F32), (8, count)).astype(BF)
    live_len = dot(lens, spread)[0:1]
    place = lax.broadcasted_iota(jnp.int32, (1, tok_rows), 1) % span
    live = place.astype(F32) < live_len
    routing = routing_ref[...]
    ids = lax.broadcasted_iota(jnp.int32, (experts, tok_rows), 0)
    named = ids == routing[0:1]
    for i in range(1, chosen):
        named = named | (ids == routing[i : i + 1])
    named = named & live
    earlier = (
        lax.broadcasted_iota(jnp.int32, (tok_rows, tok_rows), 0)
        < lax.broadcasted_iota(jnp.int32, (tok_rows, tok_rows), 1)
    ).astype(BF)
    rank = dot(jnp.where(named, 1.0, 0.0).astype(BF), earlier)
    rank = jnp.where(named, rank, -1.0).astype(BF)

    def slot_ids(shape, q):
        s = lax.broadcasted_iota(jnp.int32, shape, 0)
        k = (s // bound) % per + q * per
        peer = lax.bitwise_xor(jnp.full(shape, me, jnp.int32), k)
        return peer * local + s // rows, s % bound

    def find(q):
        owner, slot = slot_ids((slots, experts), q)
        to_expert = (owner == lax.broadcasted_iota(jnp.int32, (slots, experts), 1)).astype(BF)
        owner, slot = slot_ids((slots, tok_rows), q)
        return owner, dot(to_expert, rank) == slot.astype(F32)

    floats = tok[...].astype(F32)
    scale = lax.rsqrt(jnp.mean(floats * floats, axis=-1, keepdims=True) + eps)
    normed = (tok[:, mine].astype(F32) * scale * gain_ref[:, mine]).astype(BF)

    def remote(src, dst, send, recv, device):
        return pltpu.make_async_remote_copy(
            src_ref=src, dst_ref=dst, send_sem=send, recv_sem=recv,
            device_id=device, device_id_type=MESH,
        )

    partner = (me, other)

    def landed(ref, q):
        g, i = PLACE[q]
        return ref.at[g, :, i, 1:] if q == 0 else ref.at[g, :, i]

    def at(q, j):
        g, i = PLACE[q]
        return g, slice(None), i, j

    def dispatch(k):
        q, j = k // per, k % per
        return remote(
            outgoing.at[*at(q, j)], incoming.at[*at(q, j), :, mine],
            disp_send.at[q], disp_recv.at[q], (target(k), core),
        )

    def forward(q):
        view = incoming.at[*at(q, slice(None)), :, mine]
        return remote(view, view, fwd_send.at[q], fwd_recv.at[q], partner)

    def swap(g, x):
        return remote(
            partial.at[g, x, other], theirs.at[g, x],
            part_send.at[g, x], part_recv.at[g, x], partner,
        )

    def give_back(k, x):
        q, j = k // per, k % per
        g, i = PLACE[q]
        return remote(
            returning.at[g, x, i, j], returned.at[g, x, i, j],
            ret_send.at[q], ret_recv.at[q], (target(k), core),
        )

    def fill(q):
        hit = find(q)[1]
        block = dot(jnp.where(hit, 1.0, 0.0).astype(BF), normed).astype(BF)
        block = block.reshape(local, per, bound, half)
        outgoing[at(q, slice(None))] = block
        if q == 0:
            incoming[*at(0, 0), :, mine] = block[:, 0]

    def send(q):
        for k in reversed(members(q)):
            dispatch(k).start()

    fill(3)
    pl.semaphore_wait(barrier, jnp.where(inner, 2 * per, 4 * per))

    @pl.when(inner)
    def _():
        send(3)

    @pl.when(jnp.logical_not(inner))
    def _():
        greet(ready, 1)
        greet(ready, 2)

    fill(0)
    send(0)
    fill(1)

    @pl.when(jnp.logical_not(inner))
    def _():
        send(3)
        send(1)

    fill(2)

    @pl.when(jnp.logical_not(inner))
    def _():
        send(2)

    for q in range(PARTS):
        owner, hit = find(q)
        value = jnp.zeros((slots, tok_rows), F32)
        for i in range(chosen):
            value = jnp.where(owner == routing[i : i + 1], weights_ref[i : i + 1], value)
        value = jnp.where(hit, value, 0.0).T
        high = value.astype(BF)
        comb[q, :, :slots] = high
        comb[q, :, slots:] = (value - high.astype(F32)).astype(BF)

    @pl.when(inner)
    def _():
        pl.semaphore_wait(ready, 2 * per)
        send(1)
        send(2)

    def arrive(q):
        view = landed(incoming, q).at[..., mine]
        remote(view, view, disp_send.at[q], disp_recv.at[q], partner).wait_recv()
        forward(q).start()

    def finish(g, x):
        swap(g, x).wait_recv()
        total = (partial[g, x, core].astype(F32) + theirs[g, x].astype(F32)).astype(BF)
        total = total.reshape(len(GROUPS[g]), per, bound, half)
        returning[g, x] = total
        if 0 in GROUPS[g]:
            i = PLACE[0][1]
            returned[g, x, i, 0] = total[i, 0]
        def answer(qs):
            for q in qs:
                for k in reversed(members(q)):
                    give_back(k, x).start()

        if g == 0:
            answer((3, 0))
            return

        @pl.when(inner)
        def _():
            answer((2, 1))

        @pl.when(jnp.logical_not(inner))
        def _():
            answer((1, 2))

    for q in GROUPS[0]:
        arrive(q)
    pending = None
    for g, qs in enumerate(GROUPS):
        for q in qs:
            forward(q).wait_recv()
        for x in range(local):
            xs = incoming[g, x].reshape(most, width)
            if g == 0:
                for i in range(3):
                    loads[x, i].wait()
            gate = dot(xs, gate_w[x])
            hidden[...] = (gate / (1.0 + jnp.exp(-gate)) * dot(xs, up_w[x])).astype(BF)
            if pending:
                finish(*pending)
            down = dot(hidden[...], down_w[x]).astype(BF)
            partial[g, x, 0] = down[:, :half]
            partial[g, x, 1] = down[:, half:]
            swap(g, x).start()
            pending = (g, x)
        if g + 1 < len(GROUPS):
            for q in GROUPS[g + 1]:
                arrive(q)
        finish(*pending)
        pending = None

    mixed = jnp.zeros((tok_rows, half), F32)
    for q in (0, 1, 3, 2):
        view = landed(returned, q)
        remote(view, view, ret_send.at[q], ret_recv.at[q], partner).wait_recv()
        values = returned[at(q, slice(None))].reshape(slots, half)
        mixed = mixed + dot(comb[q], jnp.concatenate((values, values)))
    out_ref[...] = mixed.astype(BF)
    for q in range(PARTS):
        view = landed(outgoing, q)
        remote(view, view, disp_send.at[q], disp_recv.at[q], partner).wait_send()
        view = landed(returning, q)
        remote(view, view, ret_send.at[q], ret_recv.at[q], partner).wait_send()
        forward(q).wait_send()
    for g in range(len(GROUPS)):
        for x in range(local):
            swap(g, x).wait_send()


def per_device(n, tokens, norm_gain, routing, route_weights, lengths, w_gate, w_up, w_down):
    local, width, units = w_gate.shape
    tok_rows, chosen = routing.shape
    experts = n * local
    bound = 2 * ((tok_rows * chosen + 2 * experts - 1) // (2 * experts))
    bound = (bound + TILE - 1) // TILE * TILE
    half = width // 2
    per = n // PARTS
    rows = per * bound
    groups, deep = len(GROUPS), len(GROUPS[0])
    span = tok_rows // lengths.shape[0]
    vmem = pl.BlockSpec(memory_space=pltpu.VMEM)
    hbm = pl.BlockSpec(memory_space=pltpu.HBM)
    dma = pltpu.SemaphoreType.DMA
    return pl.pallas_call(
        functools.partial(kernel, n, local, bound, span),
        out_shape=pltpu.VMEM((tok_rows, half), BF),
        in_specs=[hbm] * 8,
        out_specs=vmem,
        scratch_shapes=[
            pltpu.VMEM((1, width), F32),
            pltpu.VMEM((chosen, tok_rows), jnp.int32),
            pltpu.VMEM((chosen, tok_rows), F32),
            pltpu.VMEM((1, lengths.shape[0]), jnp.int32),
            pltpu.VMEM((tok_rows, width), BF),
            pltpu.VMEM((local, width, units), BF),
            pltpu.VMEM((local, width, units), BF),
            pltpu.VMEM((local, units, width), BF),
            pltpu.VMEM((groups, local, deep, per, bound, half), BF),
            pltpu.VMEM((groups, local, deep, per, bound, width), BF),
            pltpu.VMEM((deep * rows, units), BF),
            pltpu.VMEM((groups, local, 2, deep * rows, half), BF),
            pltpu.VMEM((groups, local, deep * rows, half), BF),
            pltpu.VMEM((groups, local, deep, per, bound, half), BF),
            pltpu.VMEM((groups, local, deep, per, bound, half), BF),
            pltpu.VMEM((PARTS, tok_rows, 2 * local * rows), BF),
            dma((4,)),
            dma,
            dma((local, 3)),
            pltpu.SemaphoreType.REGULAR,
            dma((PARTS,)),
            dma((PARTS,)),
            dma((PARTS,)),
            dma((PARTS,)),
            dma((groups, local)),
            dma((groups, local)),
            dma((PARTS,)),
            dma((PARTS,)),
        ],
        compiler_params=pltpu.CompilerParams(
            collective_id=0, has_side_effects=True, vmem_limit_bytes=66000000
        ),
    )(
        norm_gain.reshape(1, width),
        routing.T,
        route_weights.T,
        lengths.reshape(1, -1),
        tokens,
        w_gate,
        w_up,
        w_down,
    )


def solution(mesh):
    placed = (
        P("ep", None),
        P(),
        P("ep", None),
        P("ep", None),
        P("ep"),
        P("ep", None, "tp"),
        P("ep", None, "tp"),
        P("ep", "tp", None),
    )
    return jax.shard_map(
        functools.partial(per_device, mesh.shape["ep"]),
        mesh=mesh, in_specs=placed, out_specs=P("ep", "tp"), check_vma=False,
    )
```
